32 devices in a mesh: ep: 8 (over z, x), tp: 4 (over y, core).
Axes of the slice: x: 2, y: 2, z: 4, core: 2. Of those that a mesh axis runs over, the one named last changes fastest.
Arguments:
- tokens: bfloat16 [1024, 2048], P('ep'), may hold values from -6 to 6
- routing: int32 [1024, 2], P('ep'), may hold values from 0 to 7, all different within a row; in each aligned block of 128 rows (0 to 127, 128 to 255, ...) at most 56 rows name the same one
- router_weight: bfloat16 [2048, 8], replicated, may hold values from -0.125 to 0.125
- gate_weight: bfloat16 [8, 2048, 2048], P('ep', None, 'tp'), may hold values from -0.125 to 0.125
- up_weight: bfloat16 [8, 2048, 2048], P('ep', None, 'tp'), may hold values from -0.125 to 0.125
- down_weight: bfloat16 [8, 2048, 2048], P('ep', 'tp'), may hold values from -0.125 to 0.125
- cotangent: bfloat16 [1024, 2048], P('ep'), may hold values from -0.796875 to 0.796875
Outputs:
- token_grad: bfloat16 [1024, 2048], P('ep')
- router_grad: float32 [2048, 8], P('tp')
- router_rows: float32 [2048], P('tp')
- gate_grad: bfloat16 [8, 2048, 2048], P('ep', None, 'tp')
- up_grad: bfloat16 [8, 2048, 2048], P('ep', None, 'tp')
- down_grad: bfloat16 [8, 2048, 2048], P('ep', 'tp')
- gate_rows: float32 [8, 2048], P('ep')
- up_rows: float32 [8, 2048], P('ep')
- down_rows: float32 [8, 2048], P('ep', 'tp')
The draws below stay inside these ranges and needn't reach their ends.
Inputs may be any that keep to these rules, and one draw needn't show every extreme that they name: `routing`: A row's 2 experts differ. Within the rows of one index of ep (128 rows), no expert is named more than 56 times, a bound that some block reaches.
All inputs are finite; a program needn't handle non-finite values.
Results may differ from the reference program's by a relative error of at most 0.01.
Values may be sent and summed in bfloat16 or wider, within the bound.
A program may use at most 64 MiB of HBM per device.

```python
import math
import jax
import jax.numpy as jnp
import numpy as np
from jax import lax

D = 2048
FF = 2048
TOPK = 2
TOK_DEV = 128
EXPERTS = 8
TOKENS = 1024
CAP = 56
N_EP = 8


def level_of(stream_key, shape, pieces, low, high):
    gain = 1.0
    for axis_at, parts in pieces:
        steps = jax.random.uniform(jax.random.fold_in(jax.random.fold_in(stream_key, 6), axis_at), (parts,), jnp.float32, low / len(pieces), high / len(pieces))
        gain = gain * jnp.repeat(jnp.exp(steps), shape[axis_at] // parts).reshape((-1,) + (1,) * (len(shape) - 1 - axis_at))
    return gain


def shared_out(rng, own, number, rows, number_of, top, most, lean):
    sequence = jax.random.permutation(rng, number_of)
    crowded, common = shares(number_of, rows * top, most, lean, True), shares(number_of, rows * top, most, lean, False)
    places = jnp.arange(number_of)

    def named(lengths, turn):
        used = int((lengths > 0).sum())
        fixed = max(1, used // 4)
        moved = fixed + (places - fixed + turn * (used - fixed)) % max(1, number_of - fixed)
        return jnp.zeros((number_of,), jnp.int32).at[sequence[jnp.where(places < fixed, places, moved)]].set(jnp.asarray(lengths, jnp.int32))

    lengths = jnp.where(number % 4 == 0, named(crowded, number // 4), named(common, number - number // 4 - 1))
    mixed = jax.random.permutation(jax.random.fold_in(own, 3), number_of)
    donor, sink = mixed[0:number_of // 2 * 2:2], mixed[1:number_of // 2 * 2:2]
    room = jnp.minimum(lengths[donor] - 1, most - lengths[sink]) // 2
    room = jnp.where((donor == sequence[0]) | (sink == sequence[0]) | (lengths[sink] == 0), 0, jnp.maximum(room, 0))
    moved = jax.random.randint(jax.random.fold_in(own, 4), (number_of // 2,), 0, 1 << 20) % (room + 1)
    lengths = lengths.at[donor].add(-moved).at[sink].add(moved)
    members = jnp.searchsorted(jnp.cumsum(lengths), jnp.arange(rows * top), side="right").astype(jnp.int32)
    grid = members.reshape(top, rows).T
    grid = grid[jax.random.permutation(jax.random.fold_in(own, 1), rows)]
    turn = jax.random.randint(jax.random.fold_in(own, 2), (rows, 1), 0, top)
    return jnp.take_along_axis(grid, (jnp.arange(top)[None, :] + turn) % top, axis=1)


def shares(number_of, total, bound, lean, full):
    portions = [(1 << 20) // math.isqrt(standing ** lean) + 1 for standing in range(1, number_of + 1)]
    largest = bound if full else min(bound, max(-(-total // number_of), total * portions[0] // sum(portions)))
    least = 1 if total - largest >= number_of - 1 else 0
    holding, spare = [largest] + [least] * (number_of - 1), total - largest - least * (number_of - 1)
    while spare > 0:
        candidates = [i for i in range(1, number_of) if holding[i] < largest] or [i for i in range(1, number_of) if holding[i] < bound]
        whole, left = sum([portions[i] for i in candidates]), spare
        for i in candidates:
            extra = min(bound - holding[i], max(1, left * portions[i] // whole), spare)
            holding[i] = holding[i] + extra
            spare = spare - extra
    return np.array(holding)


def gaussian(stream_key, extent, width, reach, split=(), held_as=jnp.bfloat16):
    drawn = width * jax.random.normal(stream_key, extent, jnp.float32)
    if split:
        drawn = drawn * level_of(stream_key, extent, split, -0.22, 0.18)
    return jnp.clip(drawn, -reach, reach).astype(held_as)


def setup_inputs(seed: int = 0) -> dict:
    keys = jax.random.split(jax.random.key(seed), 8)
    tokens = gaussian(keys[0], (TOKENS, D), 1.0, 6.0, ((0, 8),))
    routing_keys = jax.random.split(jax.random.fold_in(keys[1], 1), TOKENS // TOK_DEV)
    routing_turns = jax.random.permutation(jax.random.fold_in(keys[1], 3), TOKENS // TOK_DEV)
    routing = jax.vmap(lambda own, number: shared_out(jax.random.fold_in(keys[1], 2), own, number, TOK_DEV, EXPERTS, TOPK, CAP, 2))(routing_keys, routing_turns).reshape((TOKENS, TOPK))
    router_weight = gaussian(keys[2], (D, EXPERTS), D ** -0.5, 0.125)
    gate_weight = gaussian(keys[3], (EXPERTS, D, FF), D ** -0.5, 0.125, ((0, 8), (2, 4)))
    up_weight = gaussian(keys[4], (EXPERTS, D, FF), D ** -0.5, 0.125, ((0, 8), (2, 4)))
    down_weight = gaussian(keys[5], (EXPERTS, FF, D), FF ** -0.5, 0.125, ((0, 8), (1, 4)))
    cotangent = gaussian(keys[6], (TOKENS, D), 0.1, 0.796875, ((0, 8),))
    return dict(tokens=tokens, routing=routing, router_weight=router_weight, gate_weight=gate_weight, up_weight=up_weight, down_weight=down_weight, cotangent=cotangent)


def block_slots(route_block):
    flat_ids = route_block.reshape(-1)
    onehot = (flat_ids[:, None] == jnp.arange(EXPERTS, dtype=jnp.int32)[None, :]).astype(jnp.int32)
    position = jnp.sum((jnp.cumsum(onehot, axis=0) - 1) * onehot, axis=1)
    return flat_ids, position.astype(jnp.int32)


def expert_backward(rows_in, cots_in, slot_scale, w_gate, w_up, w_down):
    pre_gate = jnp.dot(rows_in, w_gate, preferred_element_type=jnp.float32)
    pre_up = jnp.dot(rows_in, w_up, preferred_element_type=jnp.float32)
    sigmoid_gate = jax.nn.sigmoid(pre_gate)
    hidden = (pre_gate * sigmoid_gate * pre_up).astype(jnp.bfloat16)
    back_proj = lax.dot_general(cots_in, w_down, (((1,), (1,)), ((), ())), preferred_element_type=jnp.float32)
    gate_term = jnp.sum(hidden.astype(jnp.float32) * back_proj, axis=1)
    scaled = slot_scale * back_proj
    grad_up_pre = (scaled * pre_gate * sigmoid_gate).astype(jnp.bfloat16)
    grad_gate_pre = (scaled * pre_up * sigmoid_gate * (1.0 + pre_gate * (1.0 - sigmoid_gate))).astype(jnp.bfloat16)
    weighted = (slot_scale * cots_in.astype(jnp.float32)).astype(jnp.bfloat16)
    contract_rows = (((0,), (0,)), ((), ()))
    grad_down = lax.dot_general(hidden, weighted, contract_rows, preferred_element_type=jnp.float32)
    grad_gate = lax.dot_general(rows_in, grad_gate_pre, contract_rows, preferred_element_type=jnp.float32)
    grad_up = lax.dot_general(rows_in, grad_up_pre, contract_rows, preferred_element_type=jnp.float32)
    contract_hidden = (((1,), (1,)), ((), ()))
    partial_value = lax.dot_general(grad_gate_pre, w_gate, contract_hidden, preferred_element_type=jnp.float32)
    partial_value = partial_value + lax.dot_general(grad_up_pre, w_up, contract_hidden, preferred_element_type=jnp.float32)
    return partial_value, gate_term, grad_gate, grad_up, grad_down


def reference(tokens, routing, router_weight, gate_weight, up_weight, down_weight, cotangent):
    logits = jnp.dot(tokens, router_weight, preferred_element_type=jnp.float32)
    affinity = jax.nn.sigmoid(logits)
    chosen = jnp.take_along_axis(affinity, routing, axis=1)
    total_aff = jnp.sum(chosen, axis=1, keepdims=True)
    weights = chosen / total_aff
    assigns = TOKENS * TOPK
    flat_ids, positions = jax.vmap(block_slots)(routing.reshape(N_EP, TOK_DEV, TOPK))
    source = jnp.arange(N_EP, dtype=jnp.int32)[:, None]
    slot_index = ((flat_ids * N_EP + source) * CAP + positions).reshape(-1)
    slot_table = jnp.full((EXPERTS * N_EP * CAP,), assigns, jnp.int32)
    slot_table = slot_table.at[slot_index].set(jnp.arange(assigns, dtype=jnp.int32))
    slot_table = slot_table.reshape(EXPERTS, N_EP * CAP)
    zero_row = jnp.zeros((1, D), jnp.bfloat16)
    tok_pad = jnp.concatenate([tokens, zero_row], axis=0)
    cot_pad = jnp.concatenate([cotangent, zero_row], axis=0)
    weight_pad = jnp.concatenate([weights.astype(jnp.bfloat16).reshape(-1), jnp.zeros((1,), jnp.bfloat16)])

    def expert(operands):
        slot_ids, w_gate, w_up, w_down = operands
        rows_in = tok_pad[slot_ids // TOPK]
        cots_in = cot_pad[slot_ids // TOPK]
        slot_scale = weight_pad[slot_ids].astype(jnp.float32)[:, None]
        return expert_backward(rows_in, cots_in, slot_scale, w_gate, w_up, w_down)

    partial_value, gate_term, grad_gate, grad_up, grad_down = lax.map(expert, (slot_table, gate_weight, up_weight, down_weight))
    gate_rows = jnp.sum(grad_gate * grad_gate, axis=2)
    up_rows = jnp.sum(grad_up * grad_up, axis=2)
    down_rows = jnp.sum(grad_down * grad_down, axis=2)
    flat_table = slot_table.reshape(-1)
    slot_grad = jnp.zeros((assigns + 1, D), jnp.bfloat16).at[flat_table].set(partial_value.astype(jnp.bfloat16).reshape(-1, D))
    slot_gate = jnp.zeros((assigns + 1,), jnp.bfloat16).at[flat_table].set(gate_term.astype(jnp.bfloat16).reshape(-1))
    back_rows = jnp.sum(slot_grad[:assigns].astype(jnp.float32).reshape(TOKENS, TOPK, D), axis=1)
    d_weights = slot_gate[:assigns].astype(jnp.float32).reshape(TOKENS, TOPK)
    d_chosen = (d_weights - jnp.sum(d_weights * weights, axis=1, keepdims=True)) / total_aff
    d_logit = d_chosen * chosen * (1.0 - chosen)
    onehot = (routing[:, :, None] == jnp.arange(EXPERTS, dtype=jnp.int32)[None, None, :]).astype(jnp.float32)
    d_logits = jnp.sum(d_logit[:, :, None] * onehot, axis=1).astype(jnp.bfloat16)
    router_grad = lax.dot_general(tokens, d_logits, (((0,), (0,)), ((), ())), preferred_element_type=jnp.float32)
    router_rows = jnp.sum(router_grad * router_grad, axis=1)
    router_back = lax.dot_general(d_logits, router_weight, (((1,), (1,)), ((), ())), preferred_element_type=jnp.float32)
    token_grad = (back_rows + router_back).astype(jnp.bfloat16)
    return (token_grad, router_grad, router_rows, grad_gate.astype(jnp.bfloat16), grad_up.astype(jnp.bfloat16),
            grad_down.astype(jnp.bfloat16), gate_rows, up_rows, down_rows)
```

```python
import functools

import jax
import jax.numpy as jnp
from jax import lax
from jax.experimental import pallas as pl
from jax.experimental.pallas import tpu as pltpu
from jax.sharding import PartitionSpec as P

LANES = 128
F32 = jnp.float32
BF16 = jnp.bfloat16
ROWS_T = (((0,), (0,)), ((), ()))
COLS_T = (((1,), (1,)), ((), ()))


def barrier(n_ep, n_tp, me, tp):
    sem = pltpu.get_barrier_semaphore()
    for i in range(1, n_ep):
        pl.semaphore_signal(sem, inc=1, device_id={"ep": lax.rem(me + i, n_ep)})
    for i in range(1, n_tp):
        pl.semaphore_signal(sem, inc=1, device_id={"tp": lax.rem(tp + i, n_tp)})
    pl.semaphore_wait(sem, n_ep + n_tp - 2)


def remote(src, dst, send, recv, where):
    return pltpu.make_async_remote_copy(
        src_ref=src, dst_ref=dst, send_sem=send, recv_sem=recv, device_id=where
    )


def named_experts(routing, experts):
    ids = lax.broadcasted_iota(jnp.int32, (routing.shape[0], experts), 1)
    named = jnp.zeros(ids.shape, F32)
    for k in range(routing.shape[1]):
        named = jnp.maximum(named, (routing[:, k : k + 1] == ids).astype(F32))
    return named


def column(value, index):
    ids = lax.broadcasted_iota(jnp.int32, value.shape, 1)
    return jnp.sum(jnp.where(ids == index, value, 0.0), axis=1, keepdims=True)


def dispatch_kernel(
    dims, tok_ref, cot_ref, routing_ref, router_ref,
    rows_ref, cots_ref, scale_ref, aff_ref, pos_ref,
    stage, scale_stage, own_sem, sc_send, sc_recv, a_send, a_recv, y_send, y_recv, p_send, p_recv,
):
    n_ep, n_tp, n_batch, capacity, cap_pad, col_width = dims
    per = n_ep // n_batch
    n_y = n_tp // 2
    me = lax.axis_index("ep")
    tp = lax.axis_index("tp")
    y_at, core = tp // 2, lax.rem(tp, 2)
    partner = y_at * 2 + 1 - core
    experts = router_ref.shape[1]
    tok_count = tok_ref.shape[0]
    outs = (rows_ref, cots_ref)

    def cols(index):
        return pl.ds(pl.multiple_of(index * col_width, LANES), col_width)

    named = named_experts(routing_ref[...], experts)
    below = (
        lax.broadcasted_iota(jnp.int32, (tok_count, tok_count), 1)
        < lax.broadcasted_iota(jnp.int32, (tok_count, tok_count), 0)
    ).astype(BF16)
    pos = jnp.dot(below, named.astype(BF16), preferred_element_type=F32)
    logits = jnp.dot(tok_ref[...], router_ref[...], preferred_element_type=F32)
    aff = jax.nn.sigmoid(logits)
    total = jnp.sum(aff * named, axis=1, keepdims=True)
    weights = (aff * named / total).astype(BF16).astype(F32)
    aff_ref[...] = aff
    pos_ref[...] = pos
    token_cols = (tok_ref[:, cols(tp)], cot_ref[:, cols(tp)])
    slots = lax.broadcasted_iota(jnp.int32, (tok_count, cap_pad), 1).astype(F32)

    barrier(n_ep, n_tp, me, tp)
    for i in range(n_ep):
        dest = lax.rem(me + i, n_ep)
        pick = jnp.where(column(pos, dest) == slots, column(named, dest), 0.0)
        scale_stage[dest] = jnp.sum(pick * column(weights, dest), axis=0, keepdims=True)
        pick = pick.astype(BF16)
        for a in range(2):
            moved = lax.dot_general(pick, token_cols[a], ROWS_T, preferred_element_type=F32)
            stage[a, dest] = moved[:capacity].astype(BF16)
        for a in range(2):
            target = outs[a].at[me, :, cols(tp)]
            if i == 0:
                pltpu.make_async_copy(stage.at[a, dest], target, own_sem.at[a]).start()
            else:
                remote(
                    stage.at[a, dest], target, a_send.at[a, dest], a_recv.at[a, me], {"ep": dest}
                ).start()
        if i == 0:
            pltpu.make_async_copy(scale_stage.at[dest], scale_ref.at[me], own_sem.at[2]).start()
        else:
            remote(
                scale_stage.at[dest], scale_ref.at[me], sc_send.at[dest], sc_recv.at[me], {"ep": dest}
            ).start()

    def y_copy(a, batch, y_to):
        ref = outs[a].at[pl.ds(batch * per, per), :, cols(tp)]
        return remote(
            ref, ref, y_send.at[a, batch, y_to], y_recv.at[a, batch, y_at], {"tp": y_to * 2 + core}
        )

    def y_arrival(a, batch, y_from):
        ref = outs[a].at[pl.ds(batch * per, per), :, cols(y_from * 2 + core)]
        return remote(
            ref, ref, y_send.at[a, batch, y_from], y_recv.at[a, batch, y_from], {"tp": y_from * 2 + core}
        )

    def p_copy(a, batch, y_of):
        ref = outs[a].at[pl.ds(batch * per, per), :, cols(y_of * 2 + core)]
        return remote(ref, ref, p_send.at[a, batch, y_of], p_recv.at[a, batch, y_of], {"tp": partner})

    def p_arrival(a, batch, y_of):
        ref = outs[a].at[pl.ds(batch * per, per), :, cols(y_of * 2 + 1 - core)]
        return remote(ref, ref, p_send.at[a, batch, y_of], p_recv.at[a, batch, y_of], {"tp": partner})

    def relay(batch):
        for a in range(2):
            for j in range(1, n_y):
                y_from = lax.rem(y_at + j, n_y)
                y_arrival(a, batch, y_from).wait_recv()
                p_copy(a, batch, y_from).start()

    my_batch = me // per
    batches = [lax.rem(my_batch - i + n_batch, n_batch) for i in range(n_batch)]
    for i, batch in enumerate(batches):
        for a in range(2):
            for j in range(per):
                source = batch * per + j

                def from_other(a=a, source=source):
                    ref = outs[a].at[source, :, cols(tp)]
                    remote(
                        ref, ref, a_send.at[a, source], a_recv.at[a, source], {"ep": source}
                    ).wait_recv()

                def from_self(a=a, source=source):
                    pltpu.make_async_copy(
                        stage.at[a, source], outs[a].at[source, :, cols(tp)], own_sem.at[a]
                    ).wait()

                if per == 1:
                    (from_self if i == 0 else from_other)()
                elif i > 0:
                    from_other()
                else:
                    pl.when(source == me)(from_self)
                    pl.when(source != me)(from_other)
            for j in range(1, n_y):
                y_copy(a, batch, lax.rem(y_at + j, n_y)).start()
            p_copy(a, batch, y_at).start()
        if i > 1:
            relay(batches[i - 2])
    for batch in batches[-2:]:
        relay(batch)
    for batch in batches:
        for a in range(2):
            for j in range(n_y):
                p_arrival(a, batch, lax.rem(y_at + j, n_y)).wait_recv()
    for i in range(1, n_ep):
        other = lax.rem(me + i, n_ep)
        remote(
            scale_stage.at[other], scale_ref.at[other], sc_send.at[other], sc_recv.at[other], {"ep": other}
        ).wait()
        for a in range(2):
            remote(
                stage.at[a, other], outs[a].at[me, :, cols(tp)], a_send.at[a, other],
                a_recv.at[a, me], {"ep": other},
            ).wait_send()
    pltpu.make_async_copy(scale_stage.at[me], scale_ref.at[me], own_sem.at[2]).wait()
    for batch in batches:
        for a in range(2):
            for j in range(n_y):
                y_to = lax.rem(y_at + j, n_y)
                if j > 0:
                    y_copy(a, batch, y_to).wait_send()
                p_copy(a, batch, y_to).wait_send()


def combine_kernel(
    dims, part_ref, gate_ref, rowsq_ref, tok_ref, routing_ref, router_ref, aff_ref, pos_ref,
    token_ref, rgrad_ref, rrows_ref, rowsum_ref,
    r1, s1, r2, res, back, gate_in, gate_sum, gate_back, rowsq_in, rpart, rparts, tgrad,
    s1_send, s1_recv, s2_send, s2_recv, s3_send, s3_recv, gt_send, gt_recv, gb_send, gb_recv,
    rs_send, rs_recv, rp_send, rp_recv, ty_send, ty_recv, tp_send, tp_recv, own_sem,
):
    n_ep, n_tp, n_batch, capacity, cap_pad, col_width = dims
    per = n_ep // n_batch
    n_y = n_tp // 2
    me = lax.axis_index("ep")
    tp = lax.axis_index("tp")
    y_at, core = tp // 2, lax.rem(tp, 2)
    partner = y_at * 2 + 1 - core
    experts = router_ref.shape[1]
    tok_count = tok_ref.shape[0]

    def cols(index):
        return pl.ds(pl.multiple_of(index * col_width, LANES), col_width)

    def span(batch):
        return pl.ds(batch * per, per)

    my_batch = me // per
    batches = [lax.rem(my_batch + i + 1, n_batch) for i in range(n_batch)]
    barrier(n_ep, n_tp, me, tp)

    def first(batch, y_to):
        return remote(
            part_ref.at[span(batch), :, cols(y_to * 2 + 1 - core)], r1.at[y_to, span(batch)],
            s1_send.at[batch, y_to], s1_recv.at[batch, y_to], {"tp": partner},
        )

    def second(batch, y_to, y_from):
        return remote(
            s1.at[y_to, span(batch)], r2.at[y_from, span(batch)],
            s2_send.at[batch, y_to], s2_recv.at[batch, y_from], {"tp": y_to * 2 + core},
        )

    def third(dest, source):
        return remote(
            res.at[dest], back.at[source], s3_send.at[dest], s3_recv.at[source], {"ep": dest}
        )

    def gate_part(other, slot):
        return remote(gate_ref, gate_in.at[slot], gt_send.at[other], gt_recv.at[slot], {"tp": other})

    def gate_home(dest, source):
        return remote(
            gate_sum.at[dest], gate_back.at[source], gb_send.at[dest], gb_recv.at[source], {"ep": dest}
        )

    def squares(other, slot):
        return remote(rowsq_ref, rowsq_in.at[slot], rs_send.at[other], rs_recv.at[slot], {"tp": other})

    for i in range(1, n_tp):
        gate_part(lax.rem(tp + i, n_tp), tp).start()
    for batch in batches:
        for j in range(n_y):
            first(batch, lax.rem(y_at + n_y - 1 - j, n_y)).start()
    for i in range(1, n_tp):
        squares(lax.rem(tp + i, n_tp), tp).start()

    def reduce_core(batch):
        for j in range(n_y):
            y_to = lax.rem(y_at + n_y - 1 - j, n_y)
            first(batch, y_to).wait_recv()
            mine = part_ref[span(batch), :, cols(y_to * 2 + core)].astype(F32)
            s1[y_to, span(batch)] = (mine + r1[y_to, span(batch)].astype(F32)).astype(BF16)
            if j < n_y - 1:
                second(batch, y_to, y_at).start()

    def reduce_y(batch, is_own):
        total = s1[y_at, span(batch)].astype(F32)
        for j in range(1, n_y):
            y_from = lax.rem(y_at + j, n_y)
            second(batch, y_from, y_from).wait_recv()
            total = total + r2[y_from, span(batch)].astype(F32)
        res[span(batch)] = total.astype(BF16)
        for j in range(per):
            dest = batch * per + j

            def to_self(dest=dest):
                pltpu.make_async_copy(res.at[dest], back.at[dest], own_sem.at[0]).start()

            def to_other(dest=dest):
                third(dest, me).start()

            if per == 1:
                (to_self if is_own else to_other)()
            elif not is_own:
                to_other()
            else:
                pl.when(dest == me)(to_self)
                pl.when(dest != me)(to_other)

    for i, batch in enumerate(batches):
        reduce_core(batch)
        if i == 1:
            gate = gate_ref[...]
            for j in range(1, n_tp):
                other = lax.rem(tp + j, n_tp)
                gate_part(other, other).wait_recv()
                gate = gate + gate_in[other]
            gate_sum[...] = gate
            for j in range(1, n_ep):
                gate_home(lax.rem(me + j, n_ep), me).start()
        if i > 1:
            reduce_y(batches[i - 2], False)
    reduce_y(batches[-2], n_batch == 1)
    reduce_y(batches[-1], True)

    named = named_experts(routing_ref[...], experts)
    aff, pos = aff_ref[...], pos_ref[...]
    total = jnp.sum(aff * named, axis=1, keepdims=True)
    weights = aff * named / total
    slots = lax.broadcasted_iota(jnp.int32, (tok_count, cap_pad), 1).astype(F32)
    ids = lax.broadcasted_iota(jnp.int32, (tok_count, experts), 1)

    d_weights = jnp.zeros((tok_count, experts), F32)
    picks = []
    for i in range(n_ep):
        source = lax.rem(me + i, n_ep)
        if i == 0:
            terms = gate_sum[source]
        else:
            gate_home(source, source).wait_recv()
            terms = gate_back[source]
        terms = terms.astype(BF16).astype(F32)
        pick = jnp.where(column(pos, source) == slots, column(named, source), 0.0)
        term = jnp.sum(pick * terms, axis=1, keepdims=True)
        d_weights = jnp.where(ids == source, term, d_weights)
        picks.append(pick.astype(BF16))
    mean = jnp.sum(d_weights * weights, axis=1, keepdims=True)
    d_logits = ((d_weights - mean) / total * aff * (1.0 - aff) * named).astype(BF16)

    rpart[...] = lax.dot_general(d_logits, tok_ref[:, cols(tp)], ROWS_T, preferred_element_type=F32)

    def router_copy(dest, source):
        return remote(rpart, rparts.at[source], rp_send.at[dest], rp_recv.at[source], {"ep": dest})

    for i in range(1, n_ep):
        router_copy(lax.rem(me + i, n_ep), me).start()

    grad = lax.dot_general(
        d_logits, router_ref[pl.ds(pl.multiple_of(tp * col_width, LANES), col_width), :], COLS_T,
        preferred_element_type=F32,
    )
    for i in range(n_ep):
        source = lax.rem(me - i + n_ep, n_ep)
        if i == 0:
            pltpu.make_async_copy(res.at[me], back.at[me], own_sem.at[0]).wait()
        else:
            third(source, source).wait_recv()
        pick = picks[(n_ep - i) % n_ep][:, :capacity]
        grad = grad + jnp.dot(pick, back[source], preferred_element_type=F32)
    tgrad[...] = grad.astype(BF16)

    def to_y(y_to):
        return remote(
            tgrad, token_ref.at[:, cols(tp)], ty_send.at[y_to], ty_recv.at[y_at], {"tp": y_to * 2 + core}
        )

    def from_y(y_from):
        ref = token_ref.at[:, cols(y_from * 2 + core)]
        return remote(ref, ref, ty_send.at[y_from], ty_recv.at[y_from], {"tp": y_from * 2 + core})

    def own_pair():
        return remote(
            tgrad, token_ref.at[:, cols(tp)], tp_send.at[y_at], tp_recv.at[y_at], {"tp": partner}
        )

    def pair(y_of):
        ref = token_ref.at[:, cols(y_of * 2 + core)]
        return remote(ref, ref, tp_send.at[y_of], tp_recv.at[y_of], {"tp": partner})

    def pair_in(y_of):
        ref = token_ref.at[:, cols(y_of * 2 + 1 - core)]
        return remote(ref, ref, tp_send.at[y_of], tp_recv.at[y_of], {"tp": partner})

    for j in range(1, n_y):
        to_y(lax.rem(y_at + j, n_y)).start()
    own_pair().start()
    own = pltpu.make_async_copy(tgrad, token_ref.at[:, cols(tp)], own_sem.at[1])
    own.start()

    rgrad = rpart[...]
    for i in range(1, n_ep):
        source = lax.rem(me + i, n_ep)
        router_copy(source, source).wait_recv()
        rgrad = rgrad + rparts[source]
    rgrad_ref[...] = rgrad
    rrows_ref[...] = jnp.sum(rgrad * rgrad, axis=0, keepdims=True)
    sums = rowsq_ref[...]
    for i in range(1, n_tp):
        other = lax.rem(tp + i, n_tp)
        squares(other, other).wait_recv()
        sums = sums + rowsq_in[other]
    rowsum_ref[...] = sums

    for j in range(1, n_y):
        y_from = lax.rem(y_at + j, n_y)
        from_y(y_from).wait_recv()
        pair(y_from).start()
    for j in range(n_y):
        pair_in(lax.rem(y_at + j, n_y)).wait_recv()
    own.wait()
    own_pair().wait_send()
    for j in range(1, n_y):
        other = lax.rem(y_at + j, n_y)
        to_y(other).wait_send()
        pair(other).wait_send()
    for i in range(1, n_tp):
        other = lax.rem(tp + i, n_tp)
        gate_part(other, tp).wait_send()
        squares(other, tp).wait_send()
    for i in range(1, n_ep):
        other = lax.rem(me + i, n_ep)
        gate_home(other, me).wait_send()
        third(other, me).wait_send()
        router_copy(other, me).wait_send()
    for batch in batches:
        for j in range(n_y):
            y_to = lax.rem(y_at + j, n_y)
            first(batch, y_to).wait_send()
            if j > 0:
                second(batch, y_to, y_at).wait_send()


def expert_backward(rows_in, cots_in, slot_scale, w_gate, w_up, w_down):
    pre_gate = jnp.dot(rows_in, w_gate, preferred_element_type=F32)
    pre_up = jnp.dot(rows_in, w_up, preferred_element_type=F32)
    sigmoid_gate = jax.nn.sigmoid(pre_gate)
    hidden = (pre_gate * sigmoid_gate * pre_up).astype(BF16)
    back_proj = lax.dot_general(cots_in, w_down, COLS_T, preferred_element_type=F32)
    gate_term = jnp.sum(hidden.astype(F32) * back_proj, axis=1)
    scaled = slot_scale * back_proj
    grad_up_pre = (scaled * pre_gate * sigmoid_gate).astype(BF16)
    grad_gate_pre = (
        scaled * pre_up * sigmoid_gate * (1.0 + pre_gate * (1.0 - sigmoid_gate))
    ).astype(BF16)
    weighted = (slot_scale * cots_in.astype(F32)).astype(BF16)
    grad_down = lax.dot_general(hidden, weighted, ROWS_T, preferred_element_type=F32)
    grad_gate = lax.dot_general(rows_in, grad_gate_pre, ROWS_T, preferred_element_type=F32)
    grad_up = lax.dot_general(rows_in, grad_up_pre, ROWS_T, preferred_element_type=F32)
    partial_value = lax.dot_general(grad_gate_pre, w_gate, COLS_T, preferred_element_type=F32)
    partial_value = partial_value + lax.dot_general(
        grad_up_pre, w_up, COLS_T, preferred_element_type=F32
    )
    return partial_value.astype(BF16), gate_term, grad_gate, grad_up, grad_down


def per_device(tokens, routing, router_weight, gate_weight, up_weight, down_weight, cotangent):
    n_ep = lax.axis_size("ep")
    n_tp = lax.axis_size("tp")
    tok_count, width = tokens.shape
    top_count = routing.shape[1]
    experts = router_weight.shape[1]
    capacity = 7 * tok_count * top_count // (4 * experts)
    cap_pad = -(-capacity // LANES) * LANES
    slots = n_ep * capacity
    col_width = width // n_tp
    n_batch = min(n_ep, 8)
    n_y = n_tp // 2
    dims = (n_ep, n_tp, n_batch, capacity, cap_pad, col_width)
    vmem = pl.BlockSpec(memory_space=pltpu.VMEM)
    hbm = pl.BlockSpec(memory_space=pl.ANY)
    dma = pltpu.SemaphoreType.DMA

    rows, cots, scale, aff, pos = pl.pallas_call(
        functools.partial(dispatch_kernel, dims),
        out_shape=(
            jax.ShapeDtypeStruct((n_ep, capacity, width), BF16),
            jax.ShapeDtypeStruct((n_ep, capacity, width), BF16),
            jax.ShapeDtypeStruct((n_ep, 1, cap_pad), F32),
            jax.ShapeDtypeStruct((tok_count, experts), F32),
            jax.ShapeDtypeStruct((tok_count, experts), F32),
        ),
        in_specs=[vmem] * 4,
        out_specs=(hbm, hbm, vmem, vmem, vmem),
        scratch_shapes=[
            pltpu.VMEM((2, n_ep, capacity, col_width), BF16),
            pltpu.VMEM((n_ep, 1, cap_pad), F32),
            dma((3,)),
            dma((n_ep,)), dma((n_ep,)),
            dma((2, n_ep)), dma((2, n_ep)),
            dma((2, n_batch, n_y)), dma((2, n_batch, n_y)),
            dma((2, n_batch, n_y)), dma((2, n_batch, n_y)),
        ],
        compiler_params=pltpu.CompilerParams(collective_id=0, has_side_effects=True),
        name="dispatch",
    )(tokens, cotangent, routing, router_weight)

    slot_scale = scale[:, 0, :capacity].reshape(slots)[:, None]
    partial_value, gate_term, grad_gate, grad_up, grad_down = expert_backward(
        rows.reshape(slots, width), cots.reshape(slots, width), slot_scale,
        gate_weight[0], up_weight[0], down_weight[0],
    )
    gate_term = jnp.pad(
        gate_term.reshape(n_ep, 1, capacity), ((0, 0), (0, 0), (0, cap_pad - capacity))
    )
    row_squares = jnp.stack(
        [jnp.sum(grad_gate * grad_gate, axis=1), jnp.sum(grad_up * grad_up, axis=1)]
    ).reshape(2, width // LANES, LANES)
    down_rows = jnp.sum(grad_down * grad_down, axis=1)

    token_grad, router_grad, router_rows, row_sums = pl.pallas_call(
        functools.partial(combine_kernel, dims),
        out_shape=(
            jax.ShapeDtypeStruct((tok_count, width), BF16),
            jax.ShapeDtypeStruct((experts, col_width), F32),
            jax.ShapeDtypeStruct((1, col_width), F32),
            jax.ShapeDtypeStruct(row_squares.shape, F32),
        ),
        in_specs=[vmem] * 8,
        out_specs=(hbm, vmem, vmem, vmem),
        scratch_shapes=[
            pltpu.VMEM((n_y, n_ep, capacity, col_width), BF16),
            pltpu.VMEM((n_y, n_ep, capacity, col_width), BF16),
            pltpu.VMEM((n_y, n_ep, capacity, col_width), BF16),
            pltpu.VMEM((n_ep, capacity, col_width), BF16),
            pltpu.VMEM((n_ep, capacity, col_width), BF16),
            pltpu.VMEM((n_tp, n_ep, 1, cap_pad), F32),
            pltpu.VMEM((n_ep, 1, cap_pad), F32),
            pltpu.VMEM((n_ep, 1, cap_pad), F32),
            pltpu.VMEM((n_tp,) + row_squares.shape, F32),
            pltpu.VMEM((experts, col_width), F32),
            pltpu.VMEM((n_ep, experts, col_width), F32),
            pltpu.VMEM((tok_count, col_width), BF16),
            dma((n_batch, n_y)), dma((n_batch, n_y)),
            dma((n_batch, n_y)), dma((n_batch, n_y)),
            dma((n_ep,)), dma((n_ep,)),
            dma((n_tp,)), dma((n_tp,)),
            dma((n_ep,)), dma((n_ep,)),
            dma((n_tp,)), dma((n_tp,)),
            dma((n_ep,)), dma((n_ep,)),
            dma((n_y,)), dma((n_y,)),
            dma((n_y,)), dma((n_y,)),
            dma((2,)),
        ],
        compiler_params=pltpu.CompilerParams(collective_id=1, has_side_effects=True),
        name="combine",
    )(partial_value.reshape(n_ep, capacity, width), gate_term, row_squares, tokens, routing,
      router_weight, aff, pos)

    row_sums = row_sums.reshape(2, 1, width)
    return (
        token_grad,
        router_grad.T,
        router_rows[0],
        grad_gate.astype(BF16)[None],
        grad_up.astype(BF16)[None],
        grad_down.astype(BF16)[None],
        row_sums[0],
        row_sums[1],
        down_rows[None],
    )


def solution(mesh):
    return jax.shard_map(
        per_device,
        mesh=mesh,
        in_specs=(
            P("ep", None),
            P("ep", None),
            P(),
            P("ep", None, "tp"),
            P("ep", None, "tp"),
            P("ep", "tp", None),
            P("ep", None),
        ),
        out_specs=(
            P("ep", None),
            P("tp", None),
            P("tp"),
            P("ep", None, "tp"),
            P("ep", None, "tp"),
            P("ep", "tp", None),
            P("ep", None),
            P("ep", None),
            P("ep", "tp"),
        ),
        check_vma=False,
    )
```

```python
import functools

import jax
import jax.numpy as jnp
from jax import lax
from jax.experimental import pallas as pl
from jax.experimental.pallas import tpu as pltpu
from jax.sharding import PartitionSpec as P

LANES = 128
F32 = jnp.float32
BF16 = jnp.bfloat16
ROWS_T = (((0,), (0,)), ((), ()))
COLS_T = (((1,), (1,)), ((), ()))


def barrier(n_ep, n_tp, me, tp):
    sem = pltpu.get_barrier_semaphore()
    for i in range(1, n_ep):
        pl.semaphore_signal(sem, inc=1, device_id={"ep": lax.rem(me + i, n_ep)})
    for i in range(1, n_tp):
        pl.semaphore_signal(sem, inc=1, device_id={"tp": lax.rem(tp + i, n_tp)})
    pl.semaphore_wait(sem, n_ep + n_tp - 2)


def remote(src, dst, send, recv, where):
    return pltpu.make_async_remote_copy(
        src_ref=src, dst_ref=dst, send_sem=send, recv_sem=recv, device_id=where
    )


def named_experts(routing, experts):
    ids = lax.broadcasted_iota(jnp.int32, (experts, routing.shape[1]), 0)
    named = jnp.zeros(ids.shape, F32)
    for k in range(routing.shape[0]):
        named = jnp.maximum(named, (routing[k : k + 1, :] == ids).astype(F32))
    return named.T


def column(value, index):
    ids = lax.broadcasted_iota(jnp.int32, value.shape, 1)
    return jnp.sum(jnp.where(ids == index, value, 0.0), axis=1, keepdims=True)


def dispatch_kernel(
    dims, tok_ref, cot_ref, routing_ref, router_ref,
    rows_ref, cots_ref, scale_ref, aff_ref, pos_ref,
    stage, scale_stage, own_sem, sc_send, sc_recv, a_send, a_recv, y_send, y_recv, p_send, p_recv,
):
    n_ep, n_tp, n_batch, capacity, cap_pad, col_width = dims
    per = n_ep // n_batch
    n_y = n_tp // 2
    me = lax.axis_index("ep")
    tp = lax.axis_index("tp")
    y_at, core = tp // 2, lax.rem(tp, 2)
    partner = y_at * 2 + 1 - core
    experts = router_ref.shape[0]
    tok_count = tok_ref.shape[0]
    outs = (rows_ref, cots_ref)

    def cols(index):
        return pl.ds(pl.multiple_of(index * col_width, LANES), col_width)

    named = named_experts(routing_ref[...], experts)
    below = (
        lax.broadcasted_iota(jnp.int32, (tok_count, tok_count), 1)
        < lax.broadcasted_iota(jnp.int32, (tok_count, tok_count), 0)
    ).astype(BF16)
    pos = jnp.dot(below, named.astype(BF16), preferred_element_type=F32)
    logits = lax.dot_general(tok_ref[...], router_ref[...], COLS_T, preferred_element_type=F32)
    aff = jax.nn.sigmoid(logits)
    total = jnp.sum(aff * named, axis=1, keepdims=True)
    weights = (aff * named / total).astype(BF16).astype(F32)
    aff_ref[...] = aff
    pos_ref[...] = pos
    token_cols = (tok_ref[:, cols(tp)], cot_ref[:, cols(tp)])
    slots = lax.broadcasted_iota(jnp.int32, (tok_count, cap_pad), 1).astype(F32)

    barrier(n_ep, n_tp, me, tp)
    for i in range(n_ep):
        dest = lax.rem(me + i, n_ep)
        pick = jnp.where(column(pos, dest) == slots, column(named, dest), 0.0)
        scale_stage[dest] = jnp.sum(pick * column(weights, dest), axis=0, keepdims=True)
        pick = pick.astype(BF16)
        for a in range(2):
            moved = lax.dot_general(pick, token_cols[a], ROWS_T, preferred_element_type=F32)
            stage[a, dest] = moved[:capacity].astype(BF16)
        for a in range(2):
            target = outs[a].at[me, :, cols(tp)]
            if i == 0:
                pltpu.make_async_copy(stage.at[a, dest], target, own_sem.at[a]).start()
            else:
                remote(
                    stage.at[a, dest], target, a_send.at[a, dest], a_recv.at[a, me], {"ep": dest}
                ).start()
        if i == 0:
            pltpu.make_async_copy(scale_stage.at[dest], scale_ref.at[me], own_sem.at[2]).start()
        else:
            remote(
                scale_stage.at[dest], scale_ref.at[me], sc_send.at[dest], sc_recv.at[me], {"ep": dest}
            ).start()

    def y_copy(a, batch, y_to):
        ref = outs[a].at[pl.ds(batch * per, per), :, cols(tp)]
        return remote(
            ref, ref, y_send.at[a, batch, y_to], y_recv.at[a, batch, y_at], {"tp": y_to * 2 + core}
        )

    def y_arrival(a, batch, y_from):
        ref = outs[a].at[pl.ds(batch * per, per), :, cols(y_from * 2 + core)]
        return remote(
            ref, ref, y_send.at[a, batch, y_from], y_recv.at[a, batch, y_from], {"tp": y_from * 2 + core}
        )

    def p_copy(a, batch, y_of):
        ref = outs[a].at[pl.ds(batch * per, per), :, cols(y_of * 2 + core)]
        return remote(ref, ref, p_send.at[a, batch, y_of], p_recv.at[a, batch, y_of], {"tp": partner})

    def p_arrival(a, batch, y_of):
        ref = outs[a].at[pl.ds(batch * per, per), :, cols(y_of * 2 + 1 - core)]
        return remote(ref, ref, p_send.at[a, batch, y_of], p_recv.at[a, batch, y_of], {"tp": partner})

    def relay(batch):
        for a in range(2):
            for j in range(1, n_y):
                y_from = lax.rem(y_at + j, n_y)
                y_arrival(a, batch, y_from).wait_recv()
                p_copy(a, batch, y_from).start()

    my_batch = me // per
    batches = [lax.rem(my_batch - i + n_batch, n_batch) for i in range(n_batch)]
    for i, batch in enumerate(batches):
        for a in range(2):
            for j in range(per):
                source = batch * per + j

                def from_other(a=a, source=source):
                    ref = outs[a].at[source, :, cols(tp)]
                    remote(
                        ref, ref, a_send.at[a, source], a_recv.at[a, source], {"ep": source}
                    ).wait_recv()

                def from_self(a=a, source=source):
                    pltpu.make_async_copy(
                        stage.at[a, source], outs[a].at[source, :, cols(tp)], own_sem.at[a]
                    ).wait()

                if per == 1:
                    (from_self if i == 0 else from_other)()
                elif i > 0:
                    from_other()
                else:
                    pl.when(source == me)(from_self)
                    pl.when(source != me)(from_other)
            for j in range(1, n_y):
                y_copy(a, batch, lax.rem(y_at + j, n_y)).start()
            p_copy(a, batch, y_at).start()
        if i > 1:
            relay(batches[i - 2])
    for batch in batches[-2:]:
        relay(batch)
    for batch in batches:
        for a in range(2):
            for j in range(n_y):
                p_arrival(a, batch, lax.rem(y_at + j, n_y)).wait_recv()
    for i in range(1, n_ep):
        other = lax.rem(me + i, n_ep)
        remote(
            scale_stage.at[other], scale_ref.at[other], sc_send.at[other], sc_recv.at[other], {"ep": other}
        ).wait()
        for a in range(2):
            remote(
                stage.at[a, other], outs[a].at[me, :, cols(tp)], a_send.at[a, other],
                a_recv.at[a, me], {"ep": other},
            ).wait_send()
    pltpu.make_async_copy(scale_stage.at[me], scale_ref.at[me], own_sem.at[2]).wait()
    for batch in batches:
        for a in range(2):
            for j in range(n_y):
                y_to = lax.rem(y_at + j, n_y)
                if j > 0:
                    y_copy(a, batch, y_to).wait_send()
                p_copy(a, batch, y_to).wait_send()


def combine_kernel(
    dims, part_ref, gate_ref, rowsq_ref, tok_ref, routing_ref, router_ref, aff_ref, pos_ref,
    token_ref, rgrad_ref, rrows_ref, rowsum_ref,
    r1, s1, r2, res, back, gate_in, gate_sum, gate_back, rowsq_in, rpart, rparts, tgrad,
    s1_send, s1_recv, s2_send, s2_recv, s3_send, s3_recv, gt_send, gt_recv, gb_send, gb_recv,
    rs_send, rs_recv, rp_send, rp_recv, ty_send, ty_recv, tp_send, tp_recv, own_sem,
):
    n_ep, n_tp, n_batch, capacity, cap_pad, col_width = dims
    per = n_ep // n_batch
    n_y = n_tp // 2
    me = lax.axis_index("ep")
    tp = lax.axis_index("tp")
    y_at, core = tp // 2, lax.rem(tp, 2)
    partner = y_at * 2 + 1 - core
    experts = router_ref.shape[0]
    tok_count = tok_ref.shape[0]

    def cols(index):
        return pl.ds(pl.multiple_of(index * col_width, LANES), col_width)

    def span(batch):
        return pl.ds(batch * per, per)

    my_batch = me // per
    batches = [lax.rem(my_batch + i + 1, n_batch) for i in range(n_batch)]
    barrier(n_ep, n_tp, me, tp)

    def first(batch, y_to):
        return remote(
            part_ref.at[span(batch), :, cols(y_to * 2 + 1 - core)], r1.at[y_to, span(batch)],
            s1_send.at[batch, y_to], s1_recv.at[batch, y_to], {"tp": partner},
        )

    def second(batch, y_to, y_from):
        return remote(
            s1.at[y_to, span(batch)], r2.at[y_from, span(batch)],
            s2_send.at[batch, y_to], s2_recv.at[batch, y_from], {"tp": y_to * 2 + core},
        )

    def third(dest, source):
        return remote(
            res.at[dest], back.at[source], s3_send.at[dest], s3_recv.at[source], {"ep": dest}
        )

    def gate_part(other, slot):
        return remote(gate_ref, gate_in.at[slot], gt_send.at[other], gt_recv.at[slot], {"tp": other})

    def gate_home(dest, source):
        return remote(
            gate_sum.at[dest], gate_back.at[source], gb_send.at[dest], gb_recv.at[source], {"ep": dest}
        )

    def squares(other, slot):
        return remote(rowsq_ref, rowsq_in.at[slot], rs_send.at[other], rs_recv.at[slot], {"tp": other})

    for i in range(1, n_tp):
        gate_part(lax.rem(tp + i, n_tp), tp).start()
    for batch in batches:
        for j in range(n_y):
            first(batch, lax.rem(y_at + n_y - 1 - j, n_y)).start()
    for i in range(1, n_tp):
        squares(lax.rem(tp + i, n_tp), tp).start()

    def reduce_core(batch):
        for j in range(n_y):
            y_to = lax.rem(y_at + n_y - 1 - j, n_y)
            first(batch, y_to).wait_recv()
            mine = part_ref[span(batch), :, cols(y_to * 2 + core)].astype(F32)
            s1[y_to, span(batch)] = (mine + r1[y_to, span(batch)].astype(F32)).astype(BF16)
            if j < n_y - 1:
                second(batch, y_to, y_at).start()

    def reduce_y(batch, is_own):
        total = s1[y_at, span(batch)].astype(F32)
        for j in range(1, n_y):
            y_from = lax.rem(y_at + j, n_y)
            second(batch, y_from, y_from).wait_recv()
            total = total + r2[y_from, span(batch)].astype(F32)
        res[span(batch)] = total.astype(BF16)
        for j in range(per):
            dest = batch * per + j

            def to_self(dest=dest):
                pltpu.make_async_copy(res.at[dest], back.at[dest], own_sem.at[0]).start()

            def to_other(dest=dest):
                third(dest, me).start()

            if per == 1:
                (to_self if is_own else to_other)()
            elif not is_own:
                to_other()
            else:
                pl.when(dest == me)(to_self)
                pl.when(dest != me)(to_other)

    for i, batch in enumerate(batches):
        reduce_core(batch)
        if i == 1:
            gate = gate_ref[...]
            for j in range(1, n_tp):
                other = lax.rem(tp + j, n_tp)
                gate_part(other, other).wait_recv()
                gate = gate + gate_in[other]
            gate_sum[...] = gate
            for j in range(1, n_ep):
                gate_home(lax.rem(me + j, n_ep), me).start()
        if i > 1:
            reduce_y(batches[i - 2], False)
    reduce_y(batches[-2], n_batch == 1)
    reduce_y(batches[-1], True)

    named = named_experts(routing_ref[...], experts)
    aff, pos = aff_ref[...], pos_ref[...]
    total = jnp.sum(aff * named, axis=1, keepdims=True)
    weights = aff * named / total
    slots = lax.broadcasted_iota(jnp.int32, (tok_count, cap_pad), 1).astype(F32)
    ids = lax.broadcasted_iota(jnp.int32, (tok_count, experts), 1)

    d_weights = jnp.zeros((tok_count, experts), F32)
    picks = []
    for i in range(n_ep):
        source = lax.rem(me + i, n_ep)
        if i == 0:
            terms = gate_sum[source]
        else:
            gate_home(source, source).wait_recv()
            terms = gate_back[source]
        terms = terms.astype(BF16).astype(F32)
        pick = jnp.where(column(pos, source) == slots, column(named, source), 0.0)
        term = jnp.sum(pick * terms, axis=1, keepdims=True)
        d_weights = jnp.where(ids == source, term, d_weights)
        picks.append(pick.astype(BF16))
    mean = jnp.sum(d_weights * weights, axis=1, keepdims=True)
    d_logits = ((d_weights - mean) / total * aff * (1.0 - aff) * named).astype(BF16)

    rpart[...] = lax.dot_general(d_logits, tok_ref[:, cols(tp)], ROWS_T, preferred_element_type=F32)

    def router_copy(dest, source):
        return remote(rpart, rparts.at[source], rp_send.at[dest], rp_recv.at[source], {"ep": dest})

    for i in range(1, n_ep):
        router_copy(lax.rem(me + i, n_ep), me).start()

    grad = jnp.dot(d_logits, router_ref[:, cols(tp)], preferred_element_type=F32)
    for i in range(n_ep):
        source = lax.rem(me - i + n_ep, n_ep)
        if i == 0:
            pltpu.make_async_copy(res.at[me], back.at[me], own_sem.at[0]).wait()
        else:
            third(source, source).wait_recv()
        pick = picks[(n_ep - i) % n_ep][:, :capacity]
        grad = grad + jnp.dot(pick, back[source], preferred_element_type=F32)
    tgrad[...] = grad.astype(BF16)

    def to_y(y_to):
        return remote(
            tgrad, token_ref.at[:, cols(tp)], ty_send.at[y_to], ty_recv.at[y_at], {"tp": y_to * 2 + core}
        )

    def from_y(y_from):
        ref = token_ref.at[:, cols(y_from * 2 + core)]
        return remote(ref, ref, ty_send.at[y_from], ty_recv.at[y_from], {"tp": y_from * 2 + core})

    def own_pair():
        return remote(
            tgrad, token_ref.at[:, cols(tp)], tp_send.at[y_at], tp_recv.at[y_at], {"tp": partner}
        )

    def pair(y_of):
        ref = token_ref.at[:, cols(y_of * 2 + core)]
        return remote(ref, ref, tp_send.at[y_of], tp_recv.at[y_of], {"tp": partner})

    def pair_in(y_of):
        ref = token_ref.at[:, cols(y_of * 2 + 1 - core)]
        return remote(ref, ref, tp_send.at[y_of], tp_recv.at[y_of], {"tp": partner})

    for j in range(1, n_y):
        to_y(lax.rem(y_at + j, n_y)).start()
    own_pair().start()
    own = pltpu.make_async_copy(tgrad, token_ref.at[:, cols(tp)], own_sem.at[1])
    own.start()

    rgrad = rpart[...]
    for i in range(1, n_ep):
        source = lax.rem(me + i, n_ep)
        router_copy(source, source).wait_recv()
        rgrad = rgrad + rparts[source]
    rgrad_ref[...] = rgrad
    rrows_ref[...] = jnp.sum(rgrad * rgrad, axis=0, keepdims=True)
    sums = rowsq_ref[...]
    for i in range(1, n_tp):
        other = lax.rem(tp + i, n_tp)
        squares(other, other).wait_recv()
        sums = sums + rowsq_in[other]
    rowsum_ref[...] = sums

    for j in range(1, n_y):
        y_from = lax.rem(y_at + j, n_y)
        from_y(y_from).wait_recv()
        pair(y_from).start()
    for j in range(n_y):
        pair_in(lax.rem(y_at + j, n_y)).wait_recv()
    own.wait()
    own_pair().wait_send()
    for j in range(1, n_y):
        other = lax.rem(y_at + j, n_y)
        to_y(other).wait_send()
        pair(other).wait_send()
    for i in range(1, n_tp):
        other = lax.rem(tp + i, n_tp)
        gate_part(other, tp).wait_send()
        squares(other, tp).wait_send()
    for i in range(1, n_ep):
        other = lax.rem(me + i, n_ep)
        gate_home(other, me).wait_send()
        third(other, me).wait_send()
        router_copy(other, me).wait_send()
    for batch in batches:
        for j in range(n_y):
            y_to = lax.rem(y_at + j, n_y)
            first(batch, y_to).wait_send()
            if j > 0:
                second(batch, y_to, y_at).wait_send()


def lane_squares(value):
    squares = value * value
    total = squares[:, :LANES]
    for at in range(LANES, value.shape[1], LANES):
        total = total + squares[:, at : at + LANES]
    return total


def weight_grad_kernel(
    rows_ref, cots_ref, hidden_ref, gate_ref, up_ref, scale_ref,
    gate_out, up_out, down_out, squares_out, down_squares_out, hidden_t, down_acc,
):
    step = pl.program_id(0)

    @pl.when(step == 0)
    def _():
        hidden_t[...] = hidden_ref[...].T
        down_acc[...] = jnp.zeros_like(down_acc)

    rows_t = rows_ref[...].T
    for a, (pre, out) in enumerate(((gate_ref, gate_out), (up_ref, up_out))):
        grad = jnp.dot(rows_t, pre[...], preferred_element_type=F32)
        out[...] = grad.astype(BF16)
        squares_out[a] = jnp.sum(lane_squares(grad).T, axis=0, keepdims=True)
    weighted = (scale_ref[...] * cots_ref[...].astype(F32)).astype(BF16)
    grad = jnp.dot(hidden_t[...], weighted, preferred_element_type=F32)
    down_out[...] = grad.astype(BF16)
    down_acc[...] += lane_squares(grad)

    @pl.when(step == pl.num_programs(0) - 1)
    def _():
        down_squares_out[...] = jnp.sum(down_acc[...].T, axis=0, keepdims=True)


def expert_backward(rows_in, cots_in, slot_scale, w_gate, w_up, w_down):
    pre_gate = jnp.dot(rows_in, w_gate, preferred_element_type=F32)
    pre_up = jnp.dot(rows_in, w_up, preferred_element_type=F32)
    sigmoid_gate = jax.nn.sigmoid(pre_gate)
    hidden = (pre_gate * sigmoid_gate * pre_up).astype(BF16)
    back_proj = lax.dot_general(cots_in, w_down, COLS_T, preferred_element_type=F32)
    gate_term = jnp.sum(hidden.astype(F32) * back_proj, axis=1)
    scaled = slot_scale * back_proj
    grad_up_pre = (scaled * pre_gate * sigmoid_gate).astype(BF16)
    grad_gate_pre = (
        scaled * pre_up * sigmoid_gate * (1.0 + pre_gate * (1.0 - sigmoid_gate))
    ).astype(BF16)
    partial_value = lax.dot_general(grad_gate_pre, w_gate, COLS_T, preferred_element_type=F32)
    partial_value = partial_value + lax.dot_general(
        grad_up_pre, w_up, COLS_T, preferred_element_type=F32
    )
    return partial_value.astype(BF16), gate_term, hidden, grad_gate_pre, grad_up_pre


def per_device(tokens, routing, router_weight, gate_weight, up_weight, down_weight, cotangent):
    n_ep = lax.axis_size("ep")
    n_tp = lax.axis_size("tp")
    tok_count, width = tokens.shape
    top_count = routing.shape[1]
    experts = router_weight.shape[1]
    capacity = 7 * tok_count * top_count // (4 * experts)
    cap_pad = -(-capacity // LANES) * LANES
    slots = n_ep * capacity
    col_width = width // n_tp
    n_batch = min(n_ep, 8)
    n_y = n_tp // 2
    dims = (n_ep, n_tp, n_batch, capacity, cap_pad, col_width)
    vmem = pl.BlockSpec(memory_space=pltpu.VMEM)
    hbm = pl.BlockSpec(memory_space=pl.ANY)
    dma = pltpu.SemaphoreType.DMA

    rows, cots, scale, aff, pos = pl.pallas_call(
        functools.partial(dispatch_kernel, dims),
        out_shape=(
            jax.ShapeDtypeStruct((n_ep, capacity, width), BF16),
            jax.ShapeDtypeStruct((n_ep, capacity, width), BF16),
            jax.ShapeDtypeStruct((n_ep, 1, cap_pad), F32),
            jax.ShapeDtypeStruct((tok_count, experts), F32),
            jax.ShapeDtypeStruct((tok_count, experts), F32),
        ),
        in_specs=[vmem] * 4,
        out_specs=(hbm, hbm, vmem, vmem, vmem),
        scratch_shapes=[
            pltpu.VMEM((2, n_ep, capacity, col_width), BF16),
            pltpu.VMEM((n_ep, 1, cap_pad), F32),
            dma((3,)),
            dma((n_ep,)), dma((n_ep,)),
            dma((2, n_ep)), dma((2, n_ep)),
            dma((2, n_batch, n_y)), dma((2, n_batch, n_y)),
            dma((2, n_batch, n_y)), dma((2, n_batch, n_y)),
        ],
        compiler_params=pltpu.CompilerParams(collective_id=0, has_side_effects=True),
        name="dispatch",
    )(tokens, cotangent, routing.T, router_weight.T)

    slot_scale = scale[:, 0, :capacity].reshape(slots)[:, None]
    rows, cots = rows.reshape(slots, width), cots.reshape(slots, width)
    partial_value, gate_term, hidden, grad_gate_pre, grad_up_pre = expert_backward(
        rows, cots, slot_scale,
        gate_weight[0], up_weight[0], down_weight[0],
    )
    gate_term = jnp.pad(
        gate_term.reshape(n_ep, 1, capacity), ((0, 0), (0, 0), (0, cap_pad - capacity))
    )
    span = 2 * LANES if width % (2 * LANES) == 0 else LANES
    units = hidden.shape[1]
    whole = pl.BlockSpec((slots, units), lambda i: (0, 0))
    grad_gate, grad_up, grad_down, row_squares, down_rows = pl.pallas_call(
        weight_grad_kernel,
        grid=(width // span,),
        out_shape=(
            jax.ShapeDtypeStruct((width, units), BF16),
            jax.ShapeDtypeStruct((width, units), BF16),
            jax.ShapeDtypeStruct((units, width), BF16),
            jax.ShapeDtypeStruct((2, 1, width), F32),
            jax.ShapeDtypeStruct((1, units), F32),
        ),
        in_specs=[
            pl.BlockSpec((slots, span), lambda i: (0, i)),
            pl.BlockSpec((slots, span), lambda i: (0, i)),
            whole, whole, whole,
            pl.BlockSpec((slots, 1), lambda i: (0, 0)),
        ],
        out_specs=(
            pl.BlockSpec((span, units), lambda i: (i, 0)),
            pl.BlockSpec((span, units), lambda i: (i, 0)),
            pl.BlockSpec((units, span), lambda i: (0, i)),
            pl.BlockSpec((2, 1, span), lambda i: (0, 0, i)),
            pl.BlockSpec((1, units), lambda i: (0, 0)),
        ),
        scratch_shapes=[pltpu.VMEM((units, slots), BF16), pltpu.VMEM((units, LANES), F32)],
        compiler_params=pltpu.CompilerParams(dimension_semantics=("arbitrary",)),
        name="weight_grads",
    )(rows, cots, hidden, grad_gate_pre, grad_up_pre, slot_scale)

    token_grad, router_grad, router_rows, row_sums = pl.pallas_call(
        functools.partial(combine_kernel, dims),
        out_shape=(
            jax.ShapeDtypeStruct((tok_count, width), BF16),
            jax.ShapeDtypeStruct((experts, col_width), F32),
            jax.ShapeDtypeStruct((1, col_width), F32),
            jax.ShapeDtypeStruct(row_squares.shape, F32),
        ),
        in_specs=[vmem] * 8,
        out_specs=(hbm, vmem, vmem, vmem),
        scratch_shapes=[
            pltpu.VMEM((n_y, n_ep, capacity, col_width), BF16),
            pltpu.VMEM((n_y, n_ep, capacity, col_width), BF16),
            pltpu.VMEM((n_y, n_ep, capacity, col_width), BF16),
            pltpu.VMEM((n_ep, capacity, col_width), BF16),
            pltpu.VMEM((n_ep, capacity, col_width), BF16),
            pltpu.VMEM((n_tp, n_ep, 1, cap_pad), F32),
            pltpu.VMEM((n_ep, 1, cap_pad), F32),
            pltpu.VMEM((n_ep, 1, cap_pad), F32),
            pltpu.VMEM((n_tp,) + row_squares.shape, F32),
            pltpu.VMEM((experts, col_width), F32),
            pltpu.VMEM((n_ep, experts, col_width), F32),
            pltpu.VMEM((tok_count, col_width), BF16),
            dma((n_batch, n_y)), dma((n_batch, n_y)),
            dma((n_batch, n_y)), dma((n_batch, n_y)),
            dma((n_ep,)), dma((n_ep,)),
            dma((n_tp,)), dma((n_tp,)),
            dma((n_ep,)), dma((n_ep,)),
            dma((n_tp,)), dma((n_tp,)),
            dma((n_ep,)), dma((n_ep,)),
            dma((n_y,)), dma((n_y,)),
            dma((n_y,)), dma((n_y,)),
            dma((2,)),
        ],
        compiler_params=pltpu.CompilerParams(collective_id=1, has_side_effects=True),
        name="combine",
    )(partial_value.reshape(n_ep, capacity, width), gate_term, row_squares, tokens,
      routing.T, router_weight.T, aff, pos)

    return (
        token_grad,
        router_grad.T,
        router_rows[0],
        grad_gate[None],
        grad_up[None],
        grad_down[None],
        row_sums[0],
        row_sums[1],
        down_rows,
    )


def solution(mesh):
    return jax.shard_map(
        per_device,
        mesh=mesh,
        in_specs=(
            P("ep", None),
            P("ep", None),
            P(),
            P("ep", None, "tp"),
            P("ep", None, "tp"),
            P("ep", "tp", None),
            P("ep", None),
        ),
        out_specs=(
            P("ep", None),
            P("tp", None),
            P("tp"),
            P("ep", None, "tp"),
            P("ep", None, "tp"),
            P("ep", "tp", None),
            P("ep", None),
            P("ep", None),
            P("ep", "tp"),
        ),
        check_vma=False,
    )
```

```python
import functools

import jax
import jax.numpy as jnp
from jax import lax
from jax.experimental import pallas as pl
from jax.experimental.pallas import tpu as pltpu
from jax.sharding import PartitionSpec as P

LANES = 128
F32 = jnp.float32
BF16 = jnp.bfloat16
ROWS_T = (((0,), (0,)), ((), ()))
COLS_T = (((1,), (1,)), ((), ()))


def barrier(n_ep, n_tp, me, tp):
    sem = pltpu.get_barrier_semaphore()
    for i in range(1, n_ep):
        pl.semaphore_signal(sem, inc=1, device_id={"ep": lax.rem(me + i, n_ep)})
    for i in range(1, n_tp):
        pl.semaphore_signal(sem, inc=1, device_id={"tp": lax.rem(tp + i, n_tp)})
    pl.semaphore_wait(sem, n_ep + n_tp - 2)


def remote(src, dst, send, recv, where):
    return pltpu.make_async_remote_copy(
        src_ref=src, dst_ref=dst, send_sem=send, recv_sem=recv, device_id=where
    )


def named_experts(routing, experts):
    ids = lax.broadcasted_iota(jnp.int32, (experts, routing.shape[1]), 0)
    named = jnp.zeros(ids.shape, F32)
    for k in range(routing.shape[0]):
        named = jnp.maximum(named, (routing[k : k + 1, :] == ids).astype(F32))
    return named.T


def column(value, index):
    ids = lax.broadcasted_iota(jnp.int32, value.shape, 1)
    return jnp.sum(jnp.where(ids == index, value, 0.0), axis=1, keepdims=True)


def lane_sum(value):
    total = value[:, :LANES]
    for at in range(LANES, value.shape[1], LANES):
        total = total + value[:, at : at + LANES]
    return total


def dispatch_kernel(
    dims, tok_ref, cot_ref, routing_ref, router_ref, w_gate, w_up, w_down,
    rows_out, cots_out, aff_ref, pos_ref, hidden_ref, gate_pre_ref, up_pre_ref, part_ref, term_ref,
    column_ref,
    rows_ref, cots_ref, scale_ref, gate_v, up_v, down_v, w_sem, flush_sem,
    stage, scale_stage, own_sem, sc_send, sc_recv, a_send, a_recv, y_send, y_recv, p_send, p_recv,
):
    n_ep, n_tp, n_batch, capacity, cap_pad, col_width = dims
    per = n_ep // n_batch
    n_y = n_tp // 2
    me = lax.axis_index("ep")
    tp = lax.axis_index("tp")
    y_at, core = tp // 2, lax.rem(tp, 2)
    partner = y_at * 2 + 1 - core
    experts = router_ref.shape[0]
    tok_count = tok_ref.shape[0]
    outs = (rows_ref, cots_ref)
    results = (rows_out, cots_out)
    weight_copies = [
        pltpu.make_async_copy(src.at[0], dst, w_sem.at[n])
        for n, (src, dst) in enumerate(((w_gate, gate_v), (w_up, up_v), (w_down, down_v)))
    ]
    for copy in weight_copies:
        copy.start()
    term_ref[...] = jnp.zeros_like(term_ref)

    def cols(index):
        return pl.ds(pl.multiple_of(index * col_width, LANES), col_width)

    named = named_experts(routing_ref[...], experts)
    below = (
        lax.broadcasted_iota(jnp.int32, (tok_count, tok_count), 1)
        < lax.broadcasted_iota(jnp.int32, (tok_count, tok_count), 0)
    ).astype(BF16)
    pos = jnp.dot(below, named.astype(BF16), preferred_element_type=F32)
    logits = lax.dot_general(tok_ref[...], router_ref[...], COLS_T, preferred_element_type=F32)
    aff = jax.nn.sigmoid(logits)
    total = jnp.sum(aff * named, axis=1, keepdims=True)
    weights = (aff * named / total).astype(BF16).astype(F32)
    aff_ref[...] = aff
    pos_ref[...] = pos
    token_cols = (tok_ref[:, cols(tp)], cot_ref[:, cols(tp)])
    slots = lax.broadcasted_iota(jnp.int32, (tok_count, cap_pad), 1).astype(F32)

    barrier(n_ep, n_tp, me, tp)
    for i in range(n_ep):
        dest = lax.rem(me + i, n_ep)
        pick = jnp.where(column(pos, dest) == slots, column(named, dest), 0.0)
        scale_stage[dest] = jnp.sum(pick * column(weights, dest), axis=0, keepdims=True)
        pick = pick.astype(BF16)
        for a in range(2):
            moved = lax.dot_general(pick, token_cols[a], ROWS_T, preferred_element_type=F32)
            stage[a, dest] = moved[:capacity].astype(BF16)
        for a in range(2):
            target = outs[a].at[me, :, cols(tp)]
            if i == 0:
                pltpu.make_async_copy(stage.at[a, dest], target, own_sem.at[a]).start()
            else:
                remote(
                    stage.at[a, dest], target, a_send.at[a, dest], a_recv.at[a, me], {"ep": dest}
                ).start()
        if i == 0:
            pltpu.make_async_copy(scale_stage.at[dest], scale_ref.at[me], own_sem.at[2]).start()
        else:
            remote(
                scale_stage.at[dest], scale_ref.at[me], sc_send.at[dest], sc_recv.at[me], {"ep": dest}
            ).start()

    def y_copy(a, batch, y_to):
        ref = outs[a].at[pl.ds(batch * per, per), :, cols(tp)]
        return remote(
            ref, ref, y_send.at[a, batch, y_to], y_recv.at[a, batch, y_at], {"tp": y_to * 2 + core}
        )

    def y_arrival(a, batch, y_from):
        ref = outs[a].at[pl.ds(batch * per, per), :, cols(y_from * 2 + core)]
        return remote(
            ref, ref, y_send.at[a, batch, y_from], y_recv.at[a, batch, y_from], {"tp": y_from * 2 + core}
        )

    def p_copy(a, batch, y_of):
        ref = outs[a].at[pl.ds(batch * per, per), :, cols(y_of * 2 + core)]
        return remote(ref, ref, p_send.at[a, batch, y_of], p_recv.at[a, batch, y_of], {"tp": partner})

    def p_arrival(a, batch, y_of):
        ref = outs[a].at[pl.ds(batch * per, per), :, cols(y_of * 2 + 1 - core)]
        return remote(ref, ref, p_send.at[a, batch, y_of], p_recv.at[a, batch, y_of], {"tp": partner})

    def relay(batch):
        for a in range(2):
            for j in range(1, n_y):
                y_from = lax.rem(y_at + j, n_y)
                y_arrival(a, batch, y_from).wait_recv()
                p_copy(a, batch, y_from).start()

    my_batch = me // per

    def batch_at(i):
        return lax.rem(my_batch - i + 2 * n_batch, n_batch)

    def flush(a, batch):
        part = pl.ds(batch * per, per)
        return pltpu.make_async_copy(outs[a].at[part], results[a].at[part], flush_sem.at[a, batch])

    def arrive(batch):
        for a in range(2):
            for j in range(per):
                source = batch * per + j

                @pl.when(source == me)
                def _(a=a, source=source):
                    pltpu.make_async_copy(
                        stage.at[a, source], outs[a].at[source, :, cols(tp)], own_sem.at[a]
                    ).wait()

                @pl.when(source != me)
                def _(a=a, source=source):
                    ref = outs[a].at[source, :, cols(tp)]
                    remote(
                        ref, ref, a_send.at[a, source], a_recv.at[a, source], {"ep": source}
                    ).wait_recv()

            for j in range(1, n_y):
                y_copy(a, batch, lax.rem(y_at + j, n_y)).start()
            p_copy(a, batch, y_at).start()

    def compute(source):
        @pl.when(source == me)
        def _():
            pltpu.make_async_copy(scale_stage.at[source], scale_ref.at[source], own_sem.at[2]).wait()

        @pl.when(source != me)
        def _():
            ref = scale_ref.at[source]
            remote(ref, ref, sc_send.at[source], sc_recv.at[source], {"ep": source}).wait_recv()

        scale = jnp.broadcast_to(scale_ref[source], (8, cap_pad)).T[:capacity, 0:1]
        column_ref[source] = scale
        rows_in, cots_in = rows_ref[source], cots_ref[source]
        pre_gate = jnp.dot(rows_in, gate_v[...], preferred_element_type=F32)
        pre_up = jnp.dot(rows_in, up_v[...], preferred_element_type=F32)
        back = lax.dot_general(cots_in, down_v[...], COLS_T, preferred_element_type=F32)
        sig = jax.nn.sigmoid(pre_gate)
        hidden = (pre_gate * sig * pre_up).astype(BF16)
        hidden_ref[source] = hidden
        terms = lane_sum(hidden.astype(F32) * back)
        term_ref[source, :, :capacity] = jnp.sum(terms.T, axis=0, keepdims=True)
        scaled = scale * back
        grad_up = (scaled * pre_gate * sig).astype(BF16)
        grad_gate = (scaled * pre_up * sig * (1.0 + pre_gate * (1.0 - sig))).astype(BF16)
        up_pre_ref[source] = grad_up
        gate_pre_ref[source] = grad_gate
        part = lax.dot_general(grad_gate, gate_v[...], COLS_T, preferred_element_type=F32)
        part = part + lax.dot_general(grad_up, up_v[...], COLS_T, preferred_element_type=F32)
        part_ref[source] = part.astype(BF16)

    for copy in weight_copies:
        copy.wait()

    def step(i, carry):
        @pl.when(i < n_batch)
        def _():
            arrive(batch_at(i))

        @pl.when((i >= 1) & (i < n_batch + 1))
        def _():
            relay(batch_at(i - 1))

        @pl.when(i >= 2)
        def _():
            batch = batch_at(i - 2)
            for a in range(2):
                for j in range(n_y):
                    p_arrival(a, batch, lax.rem(y_at + j, n_y)).wait_recv()
                flush(a, batch).start()
            for j in range(per):
                compute(batch * per + j)

        return carry

    lax.fori_loop(0, n_batch + 2, step, 0)
    batches = range(n_batch)
    for i in range(1, n_ep):
        other = lax.rem(me + i, n_ep)
        remote(
            scale_stage.at[other], scale_ref.at[other], sc_send.at[other], sc_recv.at[other], {"ep": other}
        ).wait_send()
        for a in range(2):
            remote(
                stage.at[a, other], outs[a].at[me, :, cols(tp)], a_send.at[a, other],
                a_recv.at[a, me], {"ep": other},
            ).wait_send()
    for batch in batches:
        for a in range(2):
            flush(a, batch).wait()
            for j in range(n_y):
                y_to = lax.rem(y_at + j, n_y)
                if j > 0:
                    y_copy(a, batch, y_to).wait_send()
                p_copy(a, batch, y_to).wait_send()


def combine_kernel(
    dims, part_ref, gate_ref, rowsq_ref, tok_ref, routing_ref, router_ref, aff_ref, pos_ref,
    token_ref, rgrad_ref, rowsum_ref,
    r1, s1, r2, res, back, gate_in, gate_sum, gate_back, rowsq_in, rpart, rparts, tgrad,
    s1_send, s1_recv, s2_send, s2_recv, s3_send, s3_recv, gt_send, gt_recv, gb_send, gb_recv,
    rs_send, rs_recv, rp_send, rp_recv, ty_send, ty_recv, tp_send, tp_recv, own_sem,
):
    n_ep, n_tp, n_batch, capacity, cap_pad, col_width = dims
    per = n_ep // n_batch
    n_y = n_tp // 2
    me = lax.axis_index("ep")
    tp = lax.axis_index("tp")
    y_at, core = tp // 2, lax.rem(tp, 2)
    partner = y_at * 2 + 1 - core
    experts = router_ref.shape[0]
    tok_count = tok_ref.shape[0]

    def cols(index):
        return pl.ds(pl.multiple_of(index * col_width, LANES), col_width)

    def span(batch):
        return pl.ds(batch * per, per)

    my_batch = me // per
    batches = [lax.rem(my_batch + i + 1, n_batch) for i in range(n_batch)]
    barrier(n_ep, n_tp, me, tp)

    def first(batch, y_to):
        return remote(
            part_ref.at[span(batch), :, cols(y_to * 2 + 1 - core)], r1.at[y_to, span(batch)],
            s1_send.at[batch, y_to], s1_recv.at[batch, y_to], {"tp": partner},
        )

    def second(batch, y_to, y_from):
        return remote(
            s1.at[y_to, span(batch)], r2.at[y_from, span(batch)],
            s2_send.at[batch, y_to], s2_recv.at[batch, y_from], {"tp": y_to * 2 + core},
        )

    def third(dest, source):
        return remote(
            res.at[dest], back.at[source], s3_send.at[dest], s3_recv.at[source], {"ep": dest}
        )

    def gate_part(other, slot):
        return remote(gate_ref, gate_in.at[slot], gt_send.at[other], gt_recv.at[slot], {"tp": other})

    def gate_home(dest, source):
        return remote(
            gate_sum.at[dest], gate_back.at[source], gb_send.at[dest], gb_recv.at[source], {"ep": dest}
        )

    def squares(other, slot):
        return remote(rowsq_ref, rowsq_in.at[slot], rs_send.at[other], rs_recv.at[slot], {"tp": other})

    for i in range(1, n_tp):
        gate_part(lax.rem(tp + i, n_tp), tp).start()
    for batch in batches:
        for j in range(n_y):
            first(batch, lax.rem(y_at + n_y - 1 - j, n_y)).start()
    for i in range(1, n_tp):
        squares(lax.rem(tp + i, n_tp), tp).start()

    def reduce_core(batch):
        for j in range(n_y):
            y_to = lax.rem(y_at + n_y - 1 - j, n_y)
            first(batch, y_to).wait_recv()
            mine = part_ref[span(batch), :, cols(y_to * 2 + core)].astype(F32)
            s1[y_to, span(batch)] = (mine + r1[y_to, span(batch)].astype(F32)).astype(BF16)
            if j < n_y - 1:
                second(batch, y_to, y_at).start()

    def reduce_y(batch, is_own):
        total = s1[y_at, span(batch)].astype(F32)
        for j in range(1, n_y):
            y_from = lax.rem(y_at + j, n_y)
            second(batch, y_from, y_from).wait_recv()
            total = total + r2[y_from, span(batch)].astype(F32)
        res[span(batch)] = total.astype(BF16)
        for j in range(per):
            dest = batch * per + j

            def to_self(dest=dest):
                pltpu.make_async_copy(res.at[dest], back.at[dest], own_sem.at[0]).start()

            def to_other(dest=dest):
                third(dest, me).start()

            if per == 1:
                (to_self if is_own else to_other)()
            elif not is_own:
                to_other()
            else:
                pl.when(dest == me)(to_self)
                pl.when(dest != me)(to_other)

    for i, batch in enumerate(batches):
        reduce_core(batch)
        if i == 1:
            gate = gate_ref[...]
            for j in range(1, n_tp):
                other = lax.rem(tp + j, n_tp)
                gate_part(other, other).wait_recv()
                gate = gate + gate_in[other]
            gate_sum[...] = gate
            for j in range(1, n_ep):
                gate_home(lax.rem(me + j, n_ep), me).start()
        if i > 1:
            reduce_y(batches[i - 2], False)
    reduce_y(batches[-2], n_batch == 1)
    reduce_y(batches[-1], True)

    named = named_experts(routing_ref[...], experts)
    aff, pos = aff_ref[...], pos_ref[...]
    total = jnp.sum(aff * named, axis=1, keepdims=True)
    weights = aff * named / total
    slots = lax.broadcasted_iota(jnp.int32, (tok_count, cap_pad), 1).astype(F32)
    ids = lax.broadcasted_iota(jnp.int32, (tok_count, experts), 1)

    d_weights = jnp.zeros((tok_count, experts), F32)
    picks = []
    for i in range(n_ep):
        source = lax.rem(me + i, n_ep)
        if i == 0:
            terms = gate_sum[source]
        else:
            gate_home(source, source).wait_recv()
            terms = gate_back[source]
        terms = terms.astype(BF16).astype(F32)
        pick = jnp.where(column(pos, source) == slots, column(named, source), 0.0)
        term = jnp.sum(pick * terms, axis=1, keepdims=True)
        d_weights = jnp.where(ids == source, term, d_weights)
        picks.append(pick.astype(BF16))
    mean = jnp.sum(d_weights * weights, axis=1, keepdims=True)
    d_logits = ((d_weights - mean) / total * aff * (1.0 - aff) * named).astype(BF16)

    rpart[...] = lax.dot_general(d_logits, tok_ref[:, cols(tp)], ROWS_T, preferred_element_type=F32)

    def router_copy(dest, source):
        return remote(rpart, rparts.at[source], rp_send.at[dest], rp_recv.at[source], {"ep": dest})

    for i in range(1, n_ep):
        router_copy(lax.rem(me + i, n_ep), me).start()

    grad = jnp.dot(d_logits, router_ref[:, cols(tp)], preferred_element_type=F32)
    for i in range(n_ep):
        source = lax.rem(me - i + n_ep, n_ep)
        if i == 0:
            pltpu.make_async_copy(res.at[me], back.at[me], own_sem.at[0]).wait()
        else:
            third(source, source).wait_recv()
        pick = picks[(n_ep - i) % n_ep][:, :capacity]
        grad = grad + jnp.dot(pick, back[source], preferred_element_type=F32)
    tgrad[...] = grad.astype(BF16)

    def to_y(y_to):
        return remote(
            tgrad, token_ref.at[:, cols(tp)], ty_send.at[y_to], ty_recv.at[y_at], {"tp": y_to * 2 + core}
        )

    def from_y(y_from):
        ref = token_ref.at[:, cols(y_from * 2 + core)]
        return remote(ref, ref, ty_send.at[y_from], ty_recv.at[y_from], {"tp": y_from * 2 + core})

    def own_pair():
        return remote(
            tgrad, token_ref.at[:, cols(tp)], tp_send.at[y_at], tp_recv.at[y_at], {"tp": partner}
        )

    def pair(y_of):
        ref = token_ref.at[:, cols(y_of * 2 + core)]
        return remote(ref, ref, tp_send.at[y_of], tp_recv.at[y_of], {"tp": partner})

    def pair_in(y_of):
        ref = token_ref.at[:, cols(y_of * 2 + 1 - core)]
        return remote(ref, ref, tp_send.at[y_of], tp_recv.at[y_of], {"tp": partner})

    for j in range(1, n_y):
        to_y(lax.rem(y_at + j, n_y)).start()
    own_pair().start()
    own = pltpu.make_async_copy(tgrad, token_ref.at[:, cols(tp)], own_sem.at[1])
    own.start()

    rgrad = rpart[...]
    for i in range(1, n_ep):
        source = lax.rem(me + i, n_ep)
        router_copy(source, source).wait_recv()
        rgrad = rgrad + rparts[source]
    rgrad_ref[...] = rgrad
    sums = rowsq_ref[...]
    for i in range(1, n_tp):
        other = lax.rem(tp + i, n_tp)
        squares(other, other).wait_recv()
        sums = sums + rowsq_in[other]
    rowsum_ref[...] = sums

    for j in range(1, n_y):
        y_from = lax.rem(y_at + j, n_y)
        from_y(y_from).wait_recv()
        pair(y_from).start()
    for j in range(n_y):
        pair_in(lax.rem(y_at + j, n_y)).wait_recv()
    own.wait()
    own_pair().wait_send()
    for j in range(1, n_y):
        other = lax.rem(y_at + j, n_y)
        to_y(other).wait_send()
        pair(other).wait_send()
    for i in range(1, n_tp):
        other = lax.rem(tp + i, n_tp)
        gate_part(other, tp).wait_send()
        squares(other, tp).wait_send()
    for i in range(1, n_ep):
        other = lax.rem(me + i, n_ep)
        gate_home(other, me).wait_send()
        third(other, me).wait_send()
        router_copy(other, me).wait_send()
    for batch in batches:
        for j in range(n_y):
            y_to = lax.rem(y_at + j, n_y)
            first(batch, y_to).wait_send()
            if j > 0:
                second(batch, y_to, y_at).wait_send()


def weight_grad_kernel(
    rows_ref, cots_ref, hidden_ref, gate_ref, up_ref, scale_ref,
    gate_out, up_out, down_out, squares_out, down_squares_out, hidden_t, down_acc,
):
    step = pl.program_id(0)

    @pl.when(step == 0)
    def _():
        hidden_t[...] = hidden_ref[...].T
        down_acc[...] = jnp.zeros_like(down_acc)

    rows_t = rows_ref[...].T
    for a, (pre, out) in enumerate(((gate_ref, gate_out), (up_ref, up_out))):
        grad = jnp.dot(rows_t, pre[...], preferred_element_type=F32)
        out[...] = grad.astype(BF16)
        squares_out[a] = jnp.sum(lane_sum(grad * grad).T, axis=0, keepdims=True)
    weighted = (scale_ref[...] * cots_ref[...].astype(F32)).astype(BF16)
    grad = jnp.dot(hidden_t[...], weighted, preferred_element_type=F32)
    down_out[...] = grad.astype(BF16)
    down_acc[...] += lane_sum(grad * grad)

    @pl.when(step == pl.num_programs(0) - 1)
    def _():
        down_squares_out[...] = jnp.sum(down_acc[...].T, axis=0, keepdims=True)


def finish_kernel(token_ref, router_ref, sums_ref, token_out, router_out, rows_out, gate_out, up_out):
    token_out[...] = token_ref[...]
    grad = router_ref[...]
    router_out[...] = grad
    rows_out[...] = jnp.sum(grad * grad, axis=0, keepdims=True)
    gate_out[...] = sums_ref[0]
    up_out[...] = sums_ref[1]


def per_device(tokens, routing, router_weight, gate_weight, up_weight, down_weight, cotangent):
    n_ep = lax.axis_size("ep")
    n_tp = lax.axis_size("tp")
    tok_count, width = tokens.shape
    top_count = routing.shape[1]
    experts = router_weight.shape[1]
    capacity = 7 * tok_count * top_count // (4 * experts)
    cap_pad = -(-capacity // LANES) * LANES
    slots = n_ep * capacity
    col_width = width // n_tp
    n_batch = min(n_ep, 8)
    n_y = n_tp // 2
    dims = (n_ep, n_tp, n_batch, capacity, cap_pad, col_width)
    vmem = pl.BlockSpec(memory_space=pltpu.VMEM)
    hbm = pl.BlockSpec(memory_space=pl.ANY)
    dma = pltpu.SemaphoreType.DMA

    units = gate_weight.shape[2]

    def per_slot(size, dtype):
        return jax.ShapeDtypeStruct((n_ep, capacity, size), dtype)

    (rows, cots, aff, pos, hidden, grad_gate_pre, grad_up_pre, partial_value, gate_term,
     slot_scale) = pl.pallas_call(
        functools.partial(dispatch_kernel, dims),
        out_shape=(
            per_slot(width, BF16),
            per_slot(width, BF16),
            jax.ShapeDtypeStruct((tok_count, experts), F32),
            jax.ShapeDtypeStruct((tok_count, experts), F32),
            per_slot(units, BF16),
            per_slot(units, BF16),
            per_slot(units, BF16),
            per_slot(width, BF16),
            jax.ShapeDtypeStruct((n_ep, 1, cap_pad), F32),
            per_slot(1, F32),
        ),
        in_specs=[vmem] * 4 + [hbm] * 3,
        out_specs=(hbm, hbm) + (vmem,) * 8,
        scratch_shapes=[
            pltpu.VMEM((n_ep, capacity, width), BF16),
            pltpu.VMEM((n_ep, capacity, width), BF16),
            pltpu.VMEM((n_ep, 1, cap_pad), F32),
            pltpu.VMEM((width, units), BF16),
            pltpu.VMEM((width, units), BF16),
            pltpu.VMEM((units, width), BF16),
            dma((3,)), dma((2, n_batch)),
            pltpu.VMEM((2, n_ep, capacity, col_width), BF16),
            pltpu.VMEM((n_ep, 1, cap_pad), F32),
            dma((3,)),
            dma((n_ep,)), dma((n_ep,)),
            dma((2, n_ep)), dma((2, n_ep)),
            dma((2, n_batch, n_y)), dma((2, n_batch, n_y)),
            dma((2, n_batch, n_y)), dma((2, n_batch, n_y)),
        ],
        compiler_params=pltpu.CompilerParams(collective_id=0, has_side_effects=True),
        name="dispatch",
    )(tokens, cotangent, routing.T, router_weight.T, gate_weight, up_weight, down_weight)

    rows, cots, hidden, grad_gate_pre, grad_up_pre, slot_scale = (
        value.reshape(slots, -1)
        for value in (rows, cots, hidden, grad_gate_pre, grad_up_pre, slot_scale)
    )
    span = 2 * LANES if width % (2 * LANES) == 0 else LANES
    whole = pl.BlockSpec((slots, units), lambda i: (0, 0))
    grad_gate, grad_up, grad_down, row_squares, down_rows = pl.pallas_call(
        weight_grad_kernel,
        grid=(width // span,),
        out_shape=(
            jax.ShapeDtypeStruct((width, units), BF16),
            jax.ShapeDtypeStruct((width, units), BF16),
            jax.ShapeDtypeStruct((units, width), BF16),
            jax.ShapeDtypeStruct((2, 1, width), F32),
            jax.ShapeDtypeStruct((1, units), F32),
        ),
        in_specs=[
            pl.BlockSpec((slots, span), lambda i: (0, i)),
            pl.BlockSpec((slots, span), lambda i: (0, i)),
            whole, whole, whole,
            pl.BlockSpec((slots, 1), lambda i: (0, 0)),
        ],
        out_specs=(
            pl.BlockSpec((span, units), lambda i: (i, 0)),
            pl.BlockSpec((span, units), lambda i: (i, 0)),
            pl.BlockSpec((units, span), lambda i: (0, i)),
            pl.BlockSpec((2, 1, span), lambda i: (0, 0, i)),
            pl.BlockSpec((1, units), lambda i: (0, 0)),
        ),
        scratch_shapes=[pltpu.VMEM((units, slots), BF16), pltpu.VMEM((units, LANES), F32)],
        compiler_params=pltpu.CompilerParams(dimension_semantics=("arbitrary",)),
        name="weight_grads",
    )(rows, cots, hidden, grad_gate_pre, grad_up_pre, slot_scale)

    token_grad, router_grad, row_sums = pl.pallas_call(
        functools.partial(combine_kernel, dims),
        out_shape=(
            jax.ShapeDtypeStruct((tok_count, width), BF16),
            jax.ShapeDtypeStruct((experts, col_width), F32),
            jax.ShapeDtypeStruct(row_squares.shape, F32),
        ),
        in_specs=[vmem] * 8,
        out_specs=(hbm, vmem, vmem),
        scratch_shapes=[
            pltpu.VMEM((n_y, n_ep, capacity, col_width), BF16),
            pltpu.VMEM((n_y, n_ep, capacity, col_width), BF16),
            pltpu.VMEM((n_y, n_ep, capacity, col_width), BF16),
            pltpu.VMEM((n_ep, capacity, col_width), BF16),
            pltpu.VMEM((n_ep, capacity, col_width), BF16),
            pltpu.VMEM((n_tp, n_ep, 1, cap_pad), F32),
            pltpu.VMEM((n_ep, 1, cap_pad), F32),
            pltpu.VMEM((n_ep, 1, cap_pad), F32),
            pltpu.VMEM((n_tp,) + row_squares.shape, F32),
            pltpu.VMEM((experts, col_width), F32),
            pltpu.VMEM((n_ep, experts, col_width), F32),
            pltpu.VMEM((tok_count, col_width), BF16),
            dma((n_batch, n_y)), dma((n_batch, n_y)),
            dma((n_batch, n_y)), dma((n_batch, n_y)),
            dma((n_ep,)), dma((n_ep,)),
            dma((n_tp,)), dma((n_tp,)),
            dma((n_ep,)), dma((n_ep,)),
            dma((n_tp,)), dma((n_tp,)),
            dma((n_ep,)), dma((n_ep,)),
            dma((n_y,)), dma((n_y,)),
            dma((n_y,)), dma((n_y,)),
            dma((2,)),
        ],
        compiler_params=pltpu.CompilerParams(collective_id=1, has_side_effects=True),
        name="combine",
    )(partial_value, gate_term, row_squares, tokens,
      routing.T, router_weight.T, aff, pos)

    token_grad, router_grad, router_rows, gate_rows, up_rows = pl.pallas_call(
        finish_kernel,
        out_shape=(
            jax.ShapeDtypeStruct((tok_count, width), BF16),
            jax.ShapeDtypeStruct((experts, col_width), F32),
            jax.ShapeDtypeStruct((1, col_width), F32),
            jax.ShapeDtypeStruct((1, width), F32),
            jax.ShapeDtypeStruct((1, width), F32),
        ),
        in_specs=[vmem] * 3,
        out_specs=(vmem,) * 5,
        name="finish",
    )(token_grad, router_grad, row_sums)
    return (
        token_grad,
        router_grad.T,
        router_rows[0],
        grad_gate[None],
        grad_up[None],
        grad_down[None],
        gate_rows,
        up_rows,
        down_rows,
    )


def solution(mesh):
    return jax.shard_map(
        per_device,
        mesh=mesh,
        in_specs=(
            P("ep", None),
            P("ep", None),
            P(),
            P("ep", None, "tp"),
            P("ep", None, "tp"),
            P("ep", "tp", None),
            P("ep", None),
        ),
        out_specs=(
            P("ep", None),
            P("tp", None),
            P("tp"),
            P("ep", None, "tp"),
            P("ep", None, "tp"),
            P("ep", "tp", None),
            P("ep", None),
            P("ep", None),
            P("ep", "tp"),
        ),
        check_vma=False,
    )
```
